32 devices in a mesh: ep: 8 (over z, x), tp: 4 (over y, core).
Axes of the slice: x: 2, y: 2, z: 4, core: 2. Of those that a mesh axis runs over, the one named last changes fastest.
Arguments:
- tokens: bfloat16 [1024, 2048], P('ep'), may hold values from -6 to 6
- cotangent: bfloat16 [1024, 2048], P('ep'), may hold values from -1.5 to 1.5
- routes: int32 [1024, 2], P('ep'), may hold values from 0 to 3, all different within a row; in each aligned block of 128 rows (0 to 127, 128 to 255, ...) at most 96 rows name the same one
- router: bfloat16 [2048, 4], replicated, may hold values from -0.125 to 0.125
- w_gate: bfloat16 [8, 2048, 2048], P('ep', None, 'tp'), may hold values from -0.125 to 0.125
- w_up: bfloat16 [8, 2048, 2048], P('ep', None, 'tp'), may hold values from -0.125 to 0.125
- w_down: bfloat16 [8, 2048, 2048], P('ep', 'tp'), may hold values from -0.09375 to 0.09375
Outputs:
- token_grad: bfloat16 [1024, 2048], P('ep', 'tp')
- gate_grad: float32 [1024, 2], P('ep')
- grad_gate: bfloat16 [8, 2048, 2048], P('ep', None, 'tp')
- grad_up: bfloat16 [8, 2048, 2048], P('ep', None, 'tp')
- grad_down: bfloat16 [8, 2048, 2048], P('ep', 'tp')
- router_grad: float32 [2048, 4], P(('ep', 'tp'))
The draws below stay inside these ranges and needn't reach their ends.
Inputs may be any that keep to these rules, and one draw needn't show every extreme that they name: `routes`: each row names 2 different experts. In the rows of one index of ep (aligned blocks of 128 rows) no expert is named by more than 96 rows, a bound that some block reaches.
All inputs are finite; a program needn't handle non-finite values.
Results may differ from the reference program's by a relative error of at most 0.018.
Values may be sent and summed in bfloat16 or wider, within the bound.
A program may use at most 64 MiB of HBM per device.

```python
import math
import jax
import jax.numpy as jnp
import numpy as np
from jax import lax

D = 2048
FF = 4096
TOP = 2
BLOCKS = 2
TOK_EP = 128
EXPERTS = 4
TOKENS = 1024
CAP = 96
N_EP = 8
N_TP = 4


def spiked(values, key, source, target, parts, factor):
    owner, partner = [(jnp.arange(values.shape[axis_at]) // (values.shape[axis_at] // parts)).reshape([-1 if axis == axis_at else 1 for axis in range(values.ndim)]) for axis_at in (source, target)]
    chosen = jax.random.permutation(key, parts)[partner]
    strong = (owner == chosen) | (owner == (partner + parts // 2) % parts)
    return jnp.where(strong, factor * values, values)


def block_levels(stream_key, dims, pieces, least, top_value):
    def one(dim, blocks):
        steps = jax.random.uniform(jax.random.fold_in(jax.random.fold_in(stream_key, 6), dim), (blocks,), jnp.float32, least / len(pieces), top_value / len(pieces))
        return jnp.repeat(jnp.exp(steps), dims[dim] // blocks).reshape((-1,) + (1,) * (len(dims) - dim - 1))

    level = one(*pieces[0])
    for cut in pieces[1:]:
        level = level * one(*cut)
    return level


def routed_block(key, own, number, rows, number_of, top, limit, slope):
    sequence = jax.random.permutation(key, number_of)
    heavy_load, ordinary = load_shares(number_of, rows * top, limit, slope, True), load_shares(number_of, rows * top, limit, slope, False)
    places = jnp.arange(number_of)

    def named(sizes, turn):
        used = int((sizes > 0).sum())
        fixed = max(1, used // 4)
        shifted = fixed + (places - fixed + turn * (used - fixed)) % max(1, number_of - fixed)
        return jnp.zeros((number_of,), jnp.int32).at[sequence[jnp.where(places < fixed, places, shifted)]].set(jnp.asarray(sizes, jnp.int32))

    sizes = jnp.where(number % 4 == 0, named(heavy_load, number // 4), named(ordinary, number - number // 4 - 1))
    mixed = jax.random.permutation(jax.random.fold_in(own, 3), number_of)
    giver, taker = mixed[0:number_of // 2 * 2:2], mixed[1:number_of // 2 * 2:2]
    slack = jnp.minimum(sizes[giver] - 1, limit - sizes[taker]) // 2
    slack = jnp.where((giver == sequence[0]) | (taker == sequence[0]) | (sizes[taker] == 0), 0, jnp.maximum(slack, 0))
    shifted = jax.random.randint(jax.random.fold_in(own, 4), (number_of // 2,), 0, 1 << 20) % (slack + 1)
    sizes = sizes.at[giver].add(-shifted).at[taker].add(shifted)
    members = jnp.searchsorted(jnp.cumsum(sizes), jnp.arange(rows * top), side="right").astype(jnp.int32)
    table = members.reshape(top, rows).T
    table = table[jax.random.permutation(jax.random.fold_in(own, 1), rows)]
    turn = jax.random.randint(jax.random.fold_in(own, 2), (rows, 1), 0, top)
    return jnp.take_along_axis(table, (jnp.arange(top)[None, :] + turn) % top, axis=1)


def load_shares(number_of, total, most, lean, full):
    loads = [(1 << 20) // math.isqrt(standing ** lean) + 1 for standing in range(1, number_of + 1)]
    largest = most if full else min(most, max(-(-total // number_of), total * loads[0] // sum(loads)))
    least = 1 if total - largest >= number_of - 1 else 0
    holding, spare = [largest] + [least] * (number_of - 1), total - largest - least * (number_of - 1)
    while spare > 0:
        candidates = [i for i in range(1, number_of) if holding[i] < largest] or [i for i in range(1, number_of) if holding[i] < most]
        pool, left = sum([loads[i] for i in candidates]), spare
        for i in candidates:
            addition = min(most - holding[i], max(1, left * loads[i] // pool), spare)
            holding[i] = holding[i] + addition
            spare = spare - addition
    return np.array(holding)


def scatter_about(own_key, extent, spread, most, split=(), kind=jnp.bfloat16):
    drawn = spread * jax.random.normal(own_key, extent, jnp.float32)
    if split:
        drawn = drawn * block_levels(own_key, extent, split, -0.22, 0.18)
    return jnp.clip(drawn, -most, most).astype(kind)


def heavy_noise(rng, shape, deviation, bound, split, heavy, kind=jnp.bfloat16):
    entries = deviation * jax.random.normal(rng, shape, jnp.float32)
    if split:
        entries = entries * block_levels(rng, shape, split, -0.22, 0.18)
    return jnp.clip(spiked(entries, jax.random.fold_in(rng, 3), *heavy), -bound, bound).astype(kind)


def setup_inputs(seed: int = 0) -> dict:
    seeds = jax.random.split(jax.random.key(seed), 8)
    tokens = heavy_noise(seeds[0], (TOKENS, D), 1.0, 6.0, ((0, 8),), (0, 1, 8, 2.0))
    cotangent = scatter_about(seeds[1], (TOKENS, D), 0.25, 1.5, ((0, 8),))
    routes_keys = jax.random.split(jax.random.fold_in(seeds[2], 1), TOKENS // TOK_EP)
    routes_turns = jax.random.permutation(jax.random.fold_in(seeds[2], 3), TOKENS // TOK_EP)
    routes = jax.vmap(lambda own, number: routed_block(jax.random.fold_in(seeds[2], 2), own, number, TOK_EP, EXPERTS, TOP, CAP, 2))(routes_keys, routes_turns).reshape((TOKENS, TOP))
    router = scatter_about(seeds[3], (D, EXPERTS), D ** -0.5, 0.125)
    w_gate = scatter_about(seeds[4], (EXPERTS * BLOCKS, D, FF // BLOCKS), D ** -0.5, 0.125, ((0, 8), (2, 4)))
    w_up = scatter_about(seeds[5], (EXPERTS * BLOCKS, D, FF // BLOCKS), D ** -0.5, 0.125, ((0, 8), (2, 4)))
    w_down = scatter_about(seeds[6], (EXPERTS * BLOCKS, FF // BLOCKS, D), FF ** -0.5, 0.09375, ((0, 8), (1, 4)))
    return {"tokens": tokens, "cotangent": cotangent, "routes": routes, "router": router, "w_gate": w_gate, "w_up": w_up, "w_down": w_down}


def build_slots(block_routes, experts, capacity):
    flat_routes = block_routes.reshape(-1)
    labels = jnp.arange(experts, dtype=jnp.int32)
    hit_mask = (flat_routes[None, :] == labels[:, None]).astype(jnp.int32)
    rank_in = jnp.cumsum(hit_mask, axis=1, dtype=jnp.int32) - 1
    slot_ids = jnp.arange(capacity, dtype=jnp.int32)
    assigned = (hit_mask[:, None, :] == 1) & (rank_in[:, None, :] == slot_ids[None, :, None])
    return assigned.astype(jnp.float32)


def gate_pair(tokens, routes, router, experts):
    logits = jnp.dot(tokens, router, preferred_element_type=jnp.float32)
    labels = jnp.arange(experts, dtype=jnp.int32)
    picked = (routes[:, :, None] == labels[None, None, :]).astype(jnp.float32)
    chosen = jnp.sum(picked * logits[:, None, :], axis=2)
    margin = chosen[:, 0] - chosen[:, 1]
    weights = jnp.stack([jax.nn.sigmoid(margin), jax.nn.sigmoid(-margin)], axis=1)
    return picked, weights


def logit_grads(picked, weights, gate_grad):
    lead_grad = weights[:, 0] * weights[:, 1] * (gate_grad[:, 0] - gate_grad[:, 1])
    pair_grad = jnp.stack([lead_grad, -lead_grad], axis=1)
    return jnp.sum(picked * pair_grad[:, :, None], axis=1)


def expert_grads(rows_in, cot_in, gate_in, gate_weight, up_weight, down_weight):
    pre_gate = jnp.dot(rows_in, gate_weight, preferred_element_type=jnp.float32)
    pre_up = jnp.dot(rows_in, up_weight, preferred_element_type=jnp.float32)
    back_grad = lax.dot_general(cot_in, down_weight, (((1,), (1,)), ((), ())), preferred_element_type=jnp.float32)
    sig_gate = jax.nn.sigmoid(pre_gate)
    active = pre_gate * sig_gate
    hidden = (active * pre_up).astype(jnp.bfloat16)
    gate_terms = jnp.sum(hidden.astype(jnp.float32) * back_grad, axis=1)
    gate_col = gate_in.astype(jnp.float32)[:, None]
    scaled_back = gate_col * back_grad
    d_gate = (scaled_back * pre_up * sig_gate * (1.0 + pre_gate * (1.0 - sig_gate))).astype(jnp.bfloat16)
    d_up = (scaled_back * active).astype(jnp.bfloat16)
    scaled_cot = (gate_col * cot_in.astype(jnp.float32)).astype(jnp.bfloat16)
    contract_rows = (((0,), (0,)), ((), ()))
    grad_gate = lax.dot_general(rows_in, d_gate, contract_rows, preferred_element_type=jnp.float32).astype(jnp.bfloat16)
    grad_up = lax.dot_general(rows_in, d_up, contract_rows, preferred_element_type=jnp.float32).astype(jnp.bfloat16)
    grad_down = lax.dot_general(hidden, scaled_cot, contract_rows, preferred_element_type=jnp.float32).astype(jnp.bfloat16)
    return d_gate, d_up, gate_terms, grad_gate, grad_up, grad_down


def reference(tokens, cotangent, routes, router, w_gate, w_up, w_down):
    highest = lax.Precision.HIGHEST
    picked, weights = gate_pair(tokens, routes, router, EXPERTS)
    gate_send = lax.optimization_barrier(weights.astype(jnp.bfloat16)).astype(jnp.float32)
    assigned = jax.vmap(lambda block_routes: build_slots(block_routes, EXPERTS, CAP))(routes.reshape(N_EP, TOK_EP, TOP))
    by_expert = jnp.transpose(assigned, (1, 0, 2, 3))
    tok_src = tokens.reshape(N_EP, TOK_EP, D).astype(jnp.float32)
    cot_src = cotangent.reshape(N_EP, TOK_EP, D).astype(jnp.float32)
    gate_src = gate_send.reshape(N_EP, TOK_EP * TOP)
    half_ff = FF // BLOCKS
    gate_full = jnp.transpose(w_gate.reshape(EXPERTS, BLOCKS, D, half_ff), (0, 2, 1, 3)).reshape(EXPERTS, D, FF)
    up_full = jnp.transpose(w_up.reshape(EXPERTS, BLOCKS, D, half_ff), (0, 2, 1, 3)).reshape(EXPERTS, D, FF)
    down_full = w_down.reshape(EXPERTS, FF, D)
    nblocks = BLOCKS * N_TP
    block_width = FF // nblocks

    def one_expert(carry, inputs):
        dx_acc, gate_acc = carry
        slots_here, gate_weight, up_weight, down_weight = inputs
        per_token = jnp.sum(slots_here.reshape(N_EP, CAP, TOK_EP, TOP), axis=3)
        rows_in = jnp.einsum('sct,std->scd', per_token, tok_src, precision=highest).astype(jnp.bfloat16).reshape(-1, D)
        cot_in = jnp.einsum('sct,std->scd', per_token, cot_src, precision=highest).astype(jnp.bfloat16).reshape(-1, D)
        gate_in = jnp.einsum('scj,sj->sc', slots_here, gate_src, precision=highest).astype(jnp.bfloat16).reshape(-1)
        d_gate, d_up, gate_terms, grad_gate, grad_up, grad_down = expert_grads(rows_in, cot_in, gate_in, gate_weight, up_weight, down_weight)
        blocks_gate = jnp.einsum('rbh,dbh->rbd', d_gate.astype(jnp.float32).reshape(-1, nblocks, block_width),
                                 gate_weight.astype(jnp.float32).reshape(D, nblocks, block_width))
        blocks_up = jnp.einsum('rbh,dbh->rbd', d_up.astype(jnp.float32).reshape(-1, nblocks, block_width),
                               up_weight.astype(jnp.float32).reshape(D, nblocks, block_width))
        block_dx = lax.optimization_barrier((blocks_gate + blocks_up).astype(jnp.bfloat16)).astype(jnp.float32)
        pair_dx = jnp.sum(block_dx, axis=1).reshape(N_EP, CAP, D)
        dx_acc = dx_acc + jnp.einsum('sct,scd->std', per_token, pair_dx, precision=highest)
        gate_acc = gate_acc + jnp.einsum('scj,sc->sj', slots_here, gate_terms.reshape(N_EP, CAP), precision=highest)
        return (dx_acc, gate_acc), (grad_gate, grad_up, grad_down)

    start_carry = (jnp.zeros((N_EP, TOK_EP, D), jnp.float32), jnp.zeros((N_EP, TOK_EP * TOP), jnp.float32))
    (dx_acc, gate_acc), (all_gate, all_up, all_down) = lax.scan(one_expert, start_carry, (by_expert, gate_full, up_full, down_full))
    gate_grad = gate_acc.reshape(TOKENS, TOP)
    logit_grad = logit_grads(picked, weights, gate_grad)
    router_grad = jnp.dot(tokens.astype(jnp.float32).T, logit_grad, precision=highest)
    token_grad = (dx_acc.reshape(TOKENS, D) + jnp.dot(logit_grad, router.astype(jnp.float32).T, precision=highest)).astype(jnp.bfloat16)
    grad_gate = jnp.transpose(all_gate.reshape(EXPERTS, D, BLOCKS, half_ff), (0, 2, 1, 3)).reshape(EXPERTS * BLOCKS, D, half_ff)
    grad_up = jnp.transpose(all_up.reshape(EXPERTS, D, BLOCKS, half_ff), (0, 2, 1, 3)).reshape(EXPERTS * BLOCKS, D, half_ff)
    grad_down = all_down.reshape(EXPERTS * BLOCKS, half_ff, D)
    return (token_grad, gate_grad, grad_gate, grad_up, grad_down, router_grad)
```

```python
import jax
import jax.numpy as jnp
from jax import lax
from jax.sharding import PartitionSpec as P

BLOCKS = 2


def build_slots(block_routes, experts, capacity):
    flat_routes = block_routes.reshape(-1)
    labels = jnp.arange(experts, dtype=jnp.int32)
    hit_mask = (flat_routes[None, :] == labels[:, None]).astype(jnp.int32)
    rank_in = jnp.cumsum(hit_mask, axis=1, dtype=jnp.int32) - 1
    slot_ids = jnp.arange(capacity, dtype=jnp.int32)
    assigned = (hit_mask[:, None, :] == 1) & (rank_in[:, None, :] == slot_ids[None, :, None])
    return assigned.astype(jnp.float32)


def gate_pair(tokens, routes, router, experts):
    logits = jnp.dot(tokens, router, preferred_element_type=jnp.float32)
    labels = jnp.arange(experts, dtype=jnp.int32)
    picked = (routes[:, :, None] == labels[None, None, :]).astype(jnp.float32)
    chosen = jnp.sum(picked * logits[:, None, :], axis=2)
    margin = chosen[:, 0] - chosen[:, 1]
    weights = jnp.stack([jax.nn.sigmoid(margin), jax.nn.sigmoid(-margin)], axis=1)
    return (picked, weights)


def logit_grads(picked, weights, gate_grad):
    lead_grad = weights[:, 0] * weights[:, 1] * (gate_grad[:, 0] - gate_grad[:, 1])
    pair_grad = jnp.stack([lead_grad, -lead_grad], axis=1)
    return jnp.sum(picked * pair_grad[:, :, None], axis=1)


def expert_grads(rows_in, cot_in, gate_in, gate_weight, up_weight, down_weight):
    pre_gate = jnp.dot(rows_in, gate_weight, preferred_element_type=jnp.float32)
    pre_up = jnp.dot(rows_in, up_weight, preferred_element_type=jnp.float32)
    back_grad = lax.dot_general(
        cot_in, down_weight, (((1,), (1,)), ((), ())), preferred_element_type=jnp.float32
    )
    sig_gate = jax.nn.sigmoid(pre_gate)
    active = pre_gate * sig_gate
    hidden = (active * pre_up).astype(jnp.bfloat16)
    gate_terms = jnp.sum(hidden.astype(jnp.float32) * back_grad, axis=1)
    gate_col = gate_in.astype(jnp.float32)[:, None]
    scaled_back = gate_col * back_grad
    d_gate = (scaled_back * pre_up * sig_gate * (1.0 + pre_gate * (1.0 - sig_gate))).astype(
        jnp.bfloat16
    )
    d_up = (scaled_back * active).astype(jnp.bfloat16)
    scaled_cot = (gate_col * cot_in.astype(jnp.float32)).astype(jnp.bfloat16)
    contract_rows = (((0,), (0,)), ((), ()))
    grad_gate = lax.dot_general(
        rows_in, d_gate, contract_rows, preferred_element_type=jnp.float32
    ).astype(jnp.bfloat16)
    grad_up = lax.dot_general(
        rows_in, d_up, contract_rows, preferred_element_type=jnp.float32
    ).astype(jnp.bfloat16)
    grad_down = lax.dot_general(
        hidden, scaled_cot, contract_rows, preferred_element_type=jnp.float32
    ).astype(jnp.bfloat16)
    return (d_gate, d_up, gate_terms, grad_gate, grad_up, grad_down)


def spread_slabs(packed, experts, slab_count):
    widened = jnp.broadcast_to(packed[:, None], (experts, BLOCKS) + packed.shape[1:])
    return widened.reshape((slab_count,) + packed.shape[1:])


def routed_shards(tokens, cotangent, routes, router, w_gate, w_up, w_down):
    highest = lax.Precision.HIGHEST
    ep_count = lax.axis_size("ep")
    tp_count = lax.axis_size("tp")
    experts = ep_count // BLOCKS
    tok_rows, width = tokens.shape
    top_count = routes.shape[1]
    capacity = 3 * tok_rows * top_count // (2 * experts)
    col_width = width // tp_count
    tp_index = lax.axis_index("tp")
    picked, weights = gate_pair(tokens, routes, router, experts)
    assigned = build_slots(routes, experts, capacity)
    per_token = jnp.sum(assigned.reshape(experts, capacity, tok_rows, top_count), axis=3)
    token_map = per_token.astype(jnp.bfloat16)
    gate_send = weights.astype(jnp.bfloat16)
    gate_slots = jnp.einsum(
        "ecj,j->ec", assigned, gate_send.astype(jnp.float32).reshape(-1), precision=highest
    ).astype(jnp.bfloat16)
    gate_out = spread_slabs(gate_slots, experts, ep_count)

    def pack_rows(source):
        packed = jnp.einsum(
            "ect,td->ecd", token_map, source, preferred_element_type=jnp.float32
        ).astype(jnp.bfloat16)
        return spread_slabs(packed, experts, ep_count)

    tok_part = lax.dynamic_slice_in_dim(tokens, tp_index * col_width, col_width, 1)
    cot_part = lax.dynamic_slice_in_dim(cotangent, tp_index * col_width, col_width, 1)
    recv_part, recv_cot_part, recv_gate = (
        lax.all_to_all(pack_rows(tok_part), "ep", split_axis=0, concat_axis=0, tiled=True),
        lax.all_to_all(pack_rows(cot_part), "ep", split_axis=0, concat_axis=0, tiled=True),
        lax.all_to_all(gate_out, "ep", split_axis=0, concat_axis=0, tiled=True),
    )
    recv_rows, recv_cot = (
        lax.all_gather(recv_part, "tp", axis=2, tiled=True),
        lax.all_gather(recv_cot_part, "tp", axis=2, tiled=True),
    )
    rows_in = recv_rows.reshape(-1, width)
    cot_in = recv_cot.reshape(-1, width)
    gate_in = recv_gate.reshape(-1)
    d_gate, d_up, gate_terms, grad_gate, grad_up, grad_down = expert_grads(
        rows_in, cot_in, gate_in, w_gate[0], w_up[0], w_down[0]
    )
    contract_hidden = (((1,), (1,)), ((), ()))
    partial_dx = lax.dot_general(
        d_gate, w_gate[0], contract_hidden, preferred_element_type=jnp.float32
    )
    partial_dx = partial_dx + lax.dot_general(
        d_up, w_up[0], contract_hidden, preferred_element_type=jnp.float32
    )
    summed_dx = lax.psum_scatter(
        partial_dx.reshape(ep_count, capacity, width).astype(jnp.bfloat16),
        "tp",
        scatter_dimension=2,
        tiled=True,
    ).astype(jnp.float32)
    gate_sums = lax.psum(gate_terms.reshape(ep_count, capacity), "tp")
    back_dx, back_gate = (
        lax.all_to_all(
            summed_dx.astype(jnp.bfloat16), "ep", split_axis=0, concat_axis=0, tiled=True
        ).astype(summed_dx.dtype),
        lax.all_to_all(
            gate_sums.astype(jnp.bfloat16), "ep", split_axis=0, concat_axis=0, tiled=True
        ).astype(gate_sums.dtype),
    )
    slab_dx = jnp.sum(back_dx.reshape(experts, BLOCKS, capacity, col_width), axis=1)
    routed_dx = jnp.einsum("ect,ecd->td", per_token, slab_dx, precision=highest)
    slab_gate = jnp.sum(back_gate.reshape(experts, BLOCKS, capacity), axis=1)
    gate_grad = jnp.einsum("ecj,ec->j", assigned, slab_gate, precision=highest).reshape(
        tok_rows, top_count
    )
    logit_grad = logit_grads(picked, weights, gate_grad)
    router_cols = lax.dynamic_slice_in_dim(router, tp_index * col_width, col_width, 0).astype(
        jnp.float32
    )
    token_grad = (routed_dx + jnp.dot(logit_grad, router_cols.T, precision=highest)).astype(
        jnp.bfloat16
    )
    seg_rows = tok_rows // tp_count
    own_rows = lax.dynamic_slice_in_dim(tokens, tp_index * seg_rows, seg_rows, 0).astype(
        jnp.float32
    )
    own_logit = lax.dynamic_slice_in_dim(logit_grad, tp_index * seg_rows, seg_rows, 0)
    router_grad = lax.psum_scatter(
        jnp.dot(own_rows.T, own_logit, precision=highest),
        ("ep", "tp"),
        scatter_dimension=0,
        tiled=True,
    )
    return (token_grad, gate_grad, grad_gate[None], grad_up[None], grad_down[None], router_grad)


def gather_rows(part):
    rows = lax.all_gather(part, "ep", axis=0, tiled=True)
    return lax.all_gather(rows, "tp", axis=1, tiled=True)


def scatter_rows(partial):
    by_col = lax.psum_scatter(partial, "tp", scatter_dimension=1, tiled=True)
    return lax.psum_scatter(by_col, "ep", scatter_dimension=0, tiled=True)


def dense_shards(tokens, cotangent, routes, router, w_gate, w_up, w_down):
    highest = lax.Precision.HIGHEST
    ep_count = lax.axis_size("ep")
    tp_count = lax.axis_size("tp")
    experts = ep_count // BLOCKS
    tok_rows, width = tokens.shape
    col_width = width // tp_count
    ep_index = lax.axis_index("ep")
    tp_index = lax.axis_index("tp")
    expert = ep_index // BLOCKS
    w_gate, w_up, w_down = w_gate[0], w_up[0], w_down[0]

    routes_t = lax.all_gather(routes.T.astype(jnp.float32), "ep", axis=1, tiled=True)
    routes_t = routes_t.astype(jnp.int32)
    tok_part = lax.dynamic_slice_in_dim(tokens, tp_index * col_width, col_width, 1)
    cot_part = lax.dynamic_slice_in_dim(cotangent, tp_index * col_width, col_width, 1)
    tok_all = gather_rows(tok_part)
    cot_all = gather_rows(cot_part)

    logits = lax.dot_general(
        router, tok_all, (((0,), (1,)), ((), ())), preferred_element_type=jnp.float32
    )
    labels = jnp.arange(experts, dtype=jnp.int32)[:, None]
    picked = [(routes_t[k][None, :] == labels).astype(jnp.float32) for k in range(2)]
    chosen = [jnp.sum(p * logits, axis=0) for p in picked]
    margin = chosen[0] - chosen[1]
    weights = [jax.nn.sigmoid(margin), jax.nn.sigmoid(-margin)]
    sent = [w.astype(jnp.bfloat16).astype(jnp.float32) for w in weights]
    mine = [(routes_t[k] == expert).astype(jnp.float32) for k in range(2)]
    gate_col = (mine[0] * sent[0] + mine[1] * sent[1])[:, None]

    pre_gate = jnp.dot(tok_all, w_gate, preferred_element_type=jnp.float32)
    pre_up = jnp.dot(tok_all, w_up, preferred_element_type=jnp.float32)
    back_grad = lax.dot_general(
        cot_all, w_down, (((1,), (1,)), ((), ())), preferred_element_type=jnp.float32
    )
    sig_gate = jax.nn.sigmoid(pre_gate)
    active = pre_gate * sig_gate
    hidden = (active * pre_up).astype(jnp.bfloat16)
    gate_terms = jnp.sum(hidden.astype(jnp.float32) * back_grad, axis=1)
    scaled_back = gate_col * back_grad
    d_gate = (scaled_back * pre_up * sig_gate * (1.0 + pre_gate * (1.0 - sig_gate))).astype(
        jnp.bfloat16
    )
    d_up = (scaled_back * active).astype(jnp.bfloat16)
    scaled_cot = (gate_col * cot_all.astype(jnp.float32)).astype(jnp.bfloat16)

    contract_hidden = (((1,), (1,)), ((), ()))
    partial_dx = lax.dot_general(
        d_gate, w_gate, contract_hidden, preferred_element_type=jnp.float32
    )
    partial_dx = partial_dx + lax.dot_general(
        d_up, w_up, contract_hidden, preferred_element_type=jnp.float32
    )
    routed_dx = scatter_rows(partial_dx.astype(jnp.bfloat16))
    gate_sum = lax.psum(
        jnp.stack([mine[0] * gate_terms, mine[1] * gate_terms]), ("ep", "tp")
    )

    contract_rows = (((0,), (0,)), ((), ()))
    grad_gate = lax.dot_general(
        tok_all, d_gate, contract_rows, preferred_element_type=jnp.float32
    ).astype(jnp.bfloat16)
    grad_up = lax.dot_general(
        tok_all, d_up, contract_rows, preferred_element_type=jnp.float32
    ).astype(jnp.bfloat16)
    grad_down = lax.dot_general(
        hidden, scaled_cot, contract_rows, preferred_element_type=jnp.float32
    ).astype(jnp.bfloat16)

    lead = weights[0] * weights[1] * (gate_sum[0] - gate_sum[1])
    logit_grad = (picked[0] - picked[1]) * lead[None, :]
    own_logit = lax.dynamic_slice_in_dim(logit_grad, ep_index * tok_rows, tok_rows, 1)
    gate_grad = lax.dynamic_slice_in_dim(gate_sum, ep_index * tok_rows, tok_rows, 1).T
    router_cols = lax.dynamic_slice_in_dim(router, tp_index * col_width, col_width, 0)
    token_grad = (
        routed_dx.astype(jnp.float32)
        + lax.dot_general(
            own_logit,
            router_cols.astype(jnp.float32),
            (((0,), (1,)), ((), ())),
            precision=highest,
        )
    ).astype(jnp.bfloat16)
    seg = width // (ep_count * tp_count)
    own_cols = lax.dynamic_slice_in_dim(
        tok_all, (ep_index * tp_count + tp_index) * seg, seg, 1
    ).astype(jnp.float32)
    router_grad = lax.dot_general(
        logit_grad, own_cols, (((1,), (0,)), ((), ())), precision=highest
    ).T
    return (token_grad, gate_grad, grad_gate[None], grad_up[None], grad_down[None], router_grad)


def shards(tokens, cotangent, routes, router, w_gate, w_up, w_down):
    slots = 3 * routes.shape[1] * BLOCKS
    dense = slots >= lax.axis_size("ep")
    path = dense_shards if dense else routed_shards
    return path(tokens, cotangent, routes, router, w_gate, w_up, w_down)


def solution(mesh):
    placed = (
        P("ep", None),
        P("ep", None),
        P("ep", None),
        P(),
        P("ep", None, "tp"),
        P("ep", None, "tp"),
        P("ep", "tp", None),
    )
    return jax.shard_map(
        shards,
        mesh=mesh,
        in_specs=placed,
        out_specs=(
            P("ep", "tp"),
            P("ep", None),
            P("ep", None, "tp"),
            P("ep", None, "tp"),
            P("ep", "tp", None),
            P(("ep", "tp"), None),
        ),
        check_vma=False,
    )
```

```python
import jax
import jax.numpy as jnp
from jax import lax
from jax.experimental import pallas as pl
from jax.experimental.pallas import tpu as pltpu
from jax.sharding import PartitionSpec as P

BLOCKS = 2
CORES = 2
MESH = pl.DeviceIdType.MESH


def build_slots(block_routes, experts, capacity):
    flat_routes = block_routes.reshape(-1)
    labels = jnp.arange(experts, dtype=jnp.int32)
    hit_mask = (flat_routes[None, :] == labels[:, None]).astype(jnp.int32)
    rank_in = jnp.cumsum(hit_mask, axis=1, dtype=jnp.int32) - 1
    slot_ids = jnp.arange(capacity, dtype=jnp.int32)
    assigned = (hit_mask[:, None, :] == 1) & (rank_in[:, None, :] == slot_ids[None, :, None])
    return assigned.astype(jnp.float32)


def gate_pair(tokens, routes, router, experts):
    logits = jnp.dot(tokens, router, preferred_element_type=jnp.float32)
    labels = jnp.arange(experts, dtype=jnp.int32)
    picked = (routes[:, :, None] == labels[None, None, :]).astype(jnp.float32)
    chosen = jnp.sum(picked * logits[:, None, :], axis=2)
    margin = chosen[:, 0] - chosen[:, 1]
    weights = jnp.stack([jax.nn.sigmoid(margin), jax.nn.sigmoid(-margin)], axis=1)
    return (picked, weights)


def logit_grads(picked, weights, gate_grad):
    lead_grad = weights[:, 0] * weights[:, 1] * (gate_grad[:, 0] - gate_grad[:, 1])
    pair_grad = jnp.stack([lead_grad, -lead_grad], axis=1)
    return jnp.sum(picked * pair_grad[:, :, None], axis=1)


def expert_grads(rows_in, cot_in, gate_in, gate_weight, up_weight, down_weight):
    pre_gate = jnp.dot(rows_in, gate_weight, preferred_element_type=jnp.float32)
    pre_up = jnp.dot(rows_in, up_weight, preferred_element_type=jnp.float32)
    back_grad = lax.dot_general(
        cot_in, down_weight, (((1,), (1,)), ((), ())), preferred_element_type=jnp.float32
    )
    sig_gate = jax.nn.sigmoid(pre_gate)
    active = pre_gate * sig_gate
    hidden = (active * pre_up).astype(jnp.bfloat16)
    gate_terms = jnp.sum(hidden.astype(jnp.float32) * back_grad, axis=1)
    gate_col = gate_in.astype(jnp.float32)[:, None]
    scaled_back = gate_col * back_grad
    d_gate = (scaled_back * pre_up * sig_gate * (1.0 + pre_gate * (1.0 - sig_gate))).astype(
        jnp.bfloat16
    )
    d_up = (scaled_back * active).astype(jnp.bfloat16)
    scaled_cot = (gate_col * cot_in.astype(jnp.float32)).astype(jnp.bfloat16)
    contract_rows = (((0,), (0,)), ((), ()))
    grad_gate = lax.dot_general(
        rows_in, d_gate, contract_rows, preferred_element_type=jnp.float32
    ).astype(jnp.bfloat16)
    grad_up = lax.dot_general(
        rows_in, d_up, contract_rows, preferred_element_type=jnp.float32
    ).astype(jnp.bfloat16)
    grad_down = lax.dot_general(
        hidden, scaled_cot, contract_rows, preferred_element_type=jnp.float32
    ).astype(jnp.bfloat16)
    return (d_gate, d_up, gate_terms, grad_gate, grad_up, grad_down)


def spread_slabs(packed, experts, slab_count):
    widened = jnp.broadcast_to(packed[:, None], (experts, BLOCKS) + packed.shape[1:])
    return widened.reshape((slab_count,) + packed.shape[1:])


def routed_shards(tokens, cotangent, routes, router, w_gate, w_up, w_down):
    highest = lax.Precision.HIGHEST
    ep_count = lax.axis_size("ep")
    tp_count = lax.axis_size("tp")
    experts = ep_count // BLOCKS
    tok_rows, width = tokens.shape
    top_count = routes.shape[1]
    capacity = 3 * tok_rows * top_count // (2 * experts)
    col_width = width // tp_count
    tp_index = lax.axis_index("tp")
    picked, weights = gate_pair(tokens, routes, router, experts)
    assigned = build_slots(routes, experts, capacity)
    per_token = jnp.sum(assigned.reshape(experts, capacity, tok_rows, top_count), axis=3)
    token_map = per_token.astype(jnp.bfloat16)
    gate_send = weights.astype(jnp.bfloat16)
    gate_slots = jnp.einsum(
        "ecj,j->ec", assigned, gate_send.astype(jnp.float32).reshape(-1), precision=highest
    ).astype(jnp.bfloat16)
    gate_out = spread_slabs(gate_slots, experts, ep_count)

    def pack_rows(source):
        packed = jnp.einsum(
            "ect,td->ecd", token_map, source, preferred_element_type=jnp.float32
        ).astype(jnp.bfloat16)
        return spread_slabs(packed, experts, ep_count)

    tok_part = lax.dynamic_slice_in_dim(tokens, tp_index * col_width, col_width, 1)
    cot_part = lax.dynamic_slice_in_dim(cotangent, tp_index * col_width, col_width, 1)
    recv_part, recv_cot_part, recv_gate = (
        lax.all_to_all(pack_rows(tok_part), "ep", split_axis=0, concat_axis=0, tiled=True),
        lax.all_to_all(pack_rows(cot_part), "ep", split_axis=0, concat_axis=0, tiled=True),
        lax.all_to_all(gate_out, "ep", split_axis=0, concat_axis=0, tiled=True),
    )
    recv_rows, recv_cot = (
        lax.all_gather(recv_part, "tp", axis=2, tiled=True),
        lax.all_gather(recv_cot_part, "tp", axis=2, tiled=True),
    )
    rows_in = recv_rows.reshape(-1, width)
    cot_in = recv_cot.reshape(-1, width)
    gate_in = recv_gate.reshape(-1)
    d_gate, d_up, gate_terms, grad_gate, grad_up, grad_down = expert_grads(
        rows_in, cot_in, gate_in, w_gate[0], w_up[0], w_down[0]
    )
    contract_hidden = (((1,), (1,)), ((), ()))
    partial_dx = lax.dot_general(
        d_gate, w_gate[0], contract_hidden, preferred_element_type=jnp.float32
    )
    partial_dx = partial_dx + lax.dot_general(
        d_up, w_up[0], contract_hidden, preferred_element_type=jnp.float32
    )
    summed_dx = lax.psum_scatter(
        partial_dx.reshape(ep_count, capacity, width).astype(jnp.bfloat16),
        "tp",
        scatter_dimension=2,
        tiled=True,
    ).astype(jnp.float32)
    gate_sums = lax.psum(gate_terms.reshape(ep_count, capacity), "tp")
    back_dx, back_gate = (
        lax.all_to_all(
            summed_dx.astype(jnp.bfloat16), "ep", split_axis=0, concat_axis=0, tiled=True
        ).astype(summed_dx.dtype),
        lax.all_to_all(
            gate_sums.astype(jnp.bfloat16), "ep", split_axis=0, concat_axis=0, tiled=True
        ).astype(gate_sums.dtype),
    )
    slab_dx = jnp.sum(back_dx.reshape(experts, BLOCKS, capacity, col_width), axis=1)
    routed_dx = jnp.einsum("ect,ecd->td", per_token, slab_dx, precision=highest)
    slab_gate = jnp.sum(back_gate.reshape(experts, BLOCKS, capacity), axis=1)
    gate_grad = jnp.einsum("ecj,ec->j", assigned, slab_gate, precision=highest).reshape(
        tok_rows, top_count
    )
    logit_grad = logit_grads(picked, weights, gate_grad)
    router_cols = lax.dynamic_slice_in_dim(router, tp_index * col_width, col_width, 0).astype(
        jnp.float32
    )
    token_grad = (routed_dx + jnp.dot(logit_grad, router_cols.T, precision=highest)).astype(
        jnp.bfloat16
    )
    seg_rows = tok_rows // tp_count
    own_rows = lax.dynamic_slice_in_dim(tokens, tp_index * seg_rows, seg_rows, 0).astype(
        jnp.float32
    )
    own_logit = lax.dynamic_slice_in_dim(logit_grad, tp_index * seg_rows, seg_rows, 0)
    router_grad = lax.psum_scatter(
        jnp.dot(own_rows.T, own_logit, precision=highest),
        ("ep", "tp"),
        scatter_dimension=0,
        tiled=True,
    )
    return (token_grad, gate_grad, grad_gate[None], grad_up[None], grad_down[None], router_grad)


class Place:
    def __init__(self):
        self.line = lax.axis_size("ep") // BLOCKS
        ep, self.tp = lax.axis_index("ep"), lax.axis_index("tp")
        self.z, self.x = ep // BLOCKS, ep % BLOCKS
        self.y, self.c = self.tp // CORES, self.tp % CORES

    def ep(self, z, x):
        return z * BLOCKS + x

    def on_line(self, step):
        z = (self.z + step) % self.line
        return {"ep": self.ep(z, self.x), "tp": self.tp}

    def across(self):
        return {"ep": self.ep(self.z, 1 - self.x), "tp": self.tp}

    def other_plane(self):
        return {"ep": self.ep(self.z, self.x), "tp": (1 - self.y) * CORES + self.c}

    def other_core(self):
        return {"ep": self.ep(self.z, self.x), "tp": self.y * CORES + 1 - self.c}

    def greet(self):
        barrier = pltpu.get_barrier_semaphore()
        peers = [self.on_line(step) for step in range(1, self.line)]
        peers += [self.across(), self.other_plane(), self.other_core()]
        for peer in peers:
            pl.semaphore_signal(barrier, inc=1, device_id=peer, device_id_type=MESH)
        pl.semaphore_wait(barrier, len(peers))


def remote(src, dst, sems, index, peer):
    return pltpu.make_async_remote_copy(
        src_ref=src,
        dst_ref=dst,
        send_sem=sems.at[(0,) + index],
        recv_sem=sems.at[(1,) + index],
        device_id=peer,
        device_id_type=MESH,
    )


def gather_kernel(
    tok_ref, cot_ref, tok_out, cot_out, z_sems, x_sems, y_sems, c_sems, own_sems
):
    at = Place()
    line = at.line
    width = tok_ref.shape[1]
    half = width // CORES
    unit = half // 4
    ins, outs = (tok_ref, cot_ref), (tok_out, cot_out)
    own = at.ep(at.z, at.x)
    window = pl.ds(pl.multiple_of(at.c * half + at.y * unit, unit), half - unit)
    outer = pl.ds(pl.multiple_of(at.c * half + at.y * (half - unit), unit), unit)
    mine = pl.ds(pl.multiple_of(at.c * half, half), half)
    at.greet()

    started = []

    def send(src, dst, sems, index, peer):
        copy = remote(src, dst, sems, index, peer)
        copy.start()
        started.append(copy)

    for step in range(1, line):
        for i in range(2):
            send(
                ins[i].at[:, window], outs[i].at[own, :, window],
                z_sems, (step - 1, i), at.on_line(step),
            )
    for i in range(2):
        send(ins[i].at[:, window], outs[i].at[own, :, window], x_sems, (0, i), at.across())
    keep = [pltpu.make_async_copy(ins[i], outs[i].at[own], own_sems.at[i]) for i in range(2)]
    for copy in keep:
        copy.start()

    def arrived(sems, index, i, block, columns):
        ref = outs[i].at[block, :, columns]
        remote(ref, ref, sems, index, at.across()).wait_recv()

    def pass_on(block, columns, sems, index, peer, i):
        ref = outs[i].at[block, :, columns]
        send(ref, ref, sems, index, peer)

    blocks = []
    for step in range(1, line):
        block = at.ep((at.z - step + line) % line, at.x)
        blocks.append(block)
        for i in range(2):
            arrived(z_sems, (step - 1, i), i, block, window)
            pass_on(block, window, x_sems, (step, i), at.across(), i)
            pass_on(block, outer, y_sems, (step - 1, i), at.other_plane(), i)
    for step in range(line):
        block = at.ep((at.z - step + line) % line, 1 - at.x)
        blocks.append(block)
        for i in range(2):
            arrived(x_sems, (step, i), i, block, window)
            pass_on(block, outer, y_sems, (line - 1 + step, i), at.other_plane(), i)
    inner = pl.ds(pl.multiple_of(at.c * half + (1 - at.y) * (half - unit), unit), unit)
    for k, block in enumerate(blocks):
        for i in range(2):
            arrived(y_sems, (k, i), i, block, inner)
            pass_on(block, mine, c_sems, (k, i), at.other_core(), i)
    theirs = pl.ds(pl.multiple_of((1 - at.c) * half, half), half)
    for k, block in enumerate(blocks):
        for i in range(2):
            arrived(c_sems, (k, i), i, block, theirs)
    for copy in keep:
        copy.wait()
    for copy in started:
        copy.wait_send()


def gather_rows(tokens, cotangent):
    ep_count = lax.axis_size("ep")
    line = ep_count // BLOCKS
    rows, width = tokens.shape
    whole = jax.ShapeDtypeStruct((ep_count, rows, width), tokens.dtype)
    dma = pltpu.SemaphoreType.DMA
    tok_all, cot_all = pl.pallas_call(
        gather_kernel,
        out_shape=(whole, whole),
        in_specs=[pl.BlockSpec(memory_space=pltpu.VMEM)] * 2,
        out_specs=[pl.BlockSpec(memory_space=pltpu.VMEM)] * 2,
        scratch_shapes=[
            dma((2, line - 1, 2)),
            dma((2, line, 2)),
            dma((2, ep_count - 1, 2)),
            dma((2, ep_count - 1, 2)),
            dma((2,)),
        ],
        compiler_params=pltpu.CompilerParams(collective_id=0, has_side_effects=True),
    )(tokens, cotangent)
    return tok_all.reshape(-1, width), cot_all.reshape(-1, width)


def scatter_kernel(
    dx_ref, out_ref, c_recv, y_send, y_recv, x_send, x_recv, z_send, z_recv, total,
    c_sems, y_sems, x_sems, z_sems,
):
    at = Place()
    line = at.line
    part = out_ref.shape[1]

    def columns(plane, core):
        return pl.ds(pl.multiple_of((plane * CORES + core) * part, part), part)

    def f32(value):
        return value.astype(jnp.float32)

    at.greet()
    started = []

    def send(src, dst, sems, index, peer):
        copy = remote(src, dst, sems, index, peer)
        copy.start()
        started.append(copy)

    def arrived(ref, sems, index):
        remote(ref, ref, sems, index, at.across()).wait_recv()

    blocks = [
        at.ep((at.z + 1 + j) % line, x) for x in (1 - at.x, at.x) for j in range(line)
    ]
    for k, block in enumerate(blocks):
        for p in range(2):
            send(
                dx_ref.at[block, :, columns(p, 1 - at.c)], c_recv.at[k, p],
                c_sems, (k, p), at.other_core(),
            )
    for k, block in enumerate(blocks):
        for p in range(2):
            arrived(c_recv.at[k, p], c_sems, (k, p))
        y_send[k] = (
            f32(dx_ref[block, :, columns(1 - at.y, at.c)]) + f32(c_recv[k, 1 - at.y])
        ).astype(y_send.dtype)
        send(y_send.at[k], y_recv.at[k], y_sems, (k,), at.other_plane())
        total[k] = f32(dx_ref[block, :, columns(at.y, at.c)]) + f32(c_recv[k, at.y])
    for j in range(line):
        arrived(y_recv.at[j], y_sems, (j,))
        x_send[j] = (total[j] + f32(y_recv[j])).astype(x_send.dtype)
        send(x_send.at[j], x_recv.at[j], x_sems, (j,), at.across())
    for j in range(line):
        k = line + j
        arrived(y_recv.at[k], y_sems, (k,))
        arrived(x_recv.at[j], x_sems, (j,))
        summed = total[k] + f32(y_recv[k]) + f32(x_recv[j])
        if j < line - 1:
            z_send[j] = summed.astype(z_send.dtype)
            send(z_send.at[j], z_recv.at[j], z_sems, (j,), at.on_line(1 + j))
        else:
            out_ref[...] = summed
    for j in range(line - 1):
        arrived(z_recv.at[j], z_sems, (j,))
        out_ref[...] += f32(z_recv[j])
    for copy in started:
        copy.wait_send()


def scatter_rows(partial):
    ep_count, tp_count = lax.axis_size("ep"), lax.axis_size("tp")
    line = ep_count // BLOCKS
    width = partial.shape[1]
    rows, part = partial.shape[0] // ep_count, width // tp_count
    dma = pltpu.SemaphoreType.DMA

    def slots(*lead, kind=partial.dtype):
        return pltpu.VMEM(lead + (rows, part), kind)

    return pl.pallas_call(
        scatter_kernel,
        out_shape=jax.ShapeDtypeStruct((rows, part), jnp.float32),
        in_specs=[pl.BlockSpec(memory_space=pltpu.VMEM)],
        out_specs=pl.BlockSpec(memory_space=pltpu.VMEM),
        scratch_shapes=[
            slots(ep_count, 2),
            slots(ep_count),
            slots(ep_count),
            slots(line),
            slots(line),
            slots(line - 1),
            slots(line - 1),
            slots(ep_count, kind=jnp.float32),
            dma((2, ep_count, 2)),
            dma((2, ep_count)),
            dma((2, line)),
            dma((2, line - 1)),
        ],
        compiler_params=pltpu.CompilerParams(collective_id=1, has_side_effects=True),
    )(partial.reshape(ep_count, rows, width))


def dense_shards(tokens, cotangent, routes, router, w_gate, w_up, w_down):
    highest = lax.Precision.HIGHEST
    ep_count = lax.axis_size("ep")
    tp_count = lax.axis_size("tp")
    experts = ep_count // BLOCKS
    tok_rows, width = tokens.shape
    col_width = width // tp_count
    ep_index = lax.axis_index("ep")
    tp_index = lax.axis_index("tp")
    expert = ep_index // BLOCKS
    w_gate, w_up, w_down = w_gate[0], w_up[0], w_down[0]

    routes_t = lax.all_gather(routes.T.astype(jnp.float32), "ep", axis=1, tiled=True)
    routes_t = routes_t.astype(jnp.int32)
    tok_all, cot_all = gather_rows(tokens, cotangent)

    logits = lax.dot_general(
        router, tok_all, (((0,), (1,)), ((), ())), preferred_element_type=jnp.float32
    )
    labels = jnp.arange(experts, dtype=jnp.int32)[:, None]
    picked = [(routes_t[k][None, :] == labels).astype(jnp.float32) for k in range(2)]
    chosen = [jnp.sum(p * logits, axis=0) for p in picked]
    margin = chosen[0] - chosen[1]
    weights = [jax.nn.sigmoid(margin), jax.nn.sigmoid(-margin)]
    sent = [w.astype(jnp.bfloat16).astype(jnp.float32) for w in weights]
    mine = [(routes_t[k] == expert).astype(jnp.float32) for k in range(2)]
    gate_col = (mine[0] * sent[0] + mine[1] * sent[1])[:, None]

    pre_gate = jnp.dot(tok_all, w_gate, preferred_element_type=jnp.float32)
    pre_up = jnp.dot(tok_all, w_up, preferred_element_type=jnp.float32)
    back_grad = lax.dot_general(
        cot_all, w_down, (((1,), (1,)), ((), ())), preferred_element_type=jnp.float32
    )
    sig_gate = jax.nn.sigmoid(pre_gate)
    active = pre_gate * sig_gate
    hidden = (active * pre_up).astype(jnp.bfloat16)
    gate_terms = jnp.sum(hidden.astype(jnp.float32) * back_grad, axis=1)
    scaled_back = gate_col * back_grad
    d_gate = (scaled_back * pre_up * sig_gate * (1.0 + pre_gate * (1.0 - sig_gate))).astype(
        jnp.bfloat16
    )
    d_up = (scaled_back * active).astype(jnp.bfloat16)
    scaled_cot = (gate_col * cot_all.astype(jnp.float32)).astype(jnp.bfloat16)

    contract_hidden = (((1,), (1,)), ((), ()))
    partial_dx = lax.dot_general(
        d_gate, w_gate, contract_hidden, preferred_element_type=jnp.float32
    )
    partial_dx = partial_dx + lax.dot_general(
        d_up, w_up, contract_hidden, preferred_element_type=jnp.float32
    )
    routed_dx = scatter_rows(partial_dx.astype(jnp.bfloat16))
    gate_sum = lax.psum(
        jnp.stack([mine[0] * gate_terms, mine[1] * gate_terms]), ("ep", "tp")
    )

    contract_rows = (((0,), (0,)), ((), ()))
    grad_gate = lax.dot_general(
        tok_all, d_gate, contract_rows, preferred_element_type=jnp.float32
    ).astype(jnp.bfloat16)
    grad_up = lax.dot_general(
        tok_all, d_up, contract_rows, preferred_element_type=jnp.float32
    ).astype(jnp.bfloat16)
    grad_down = lax.dot_general(
        hidden, scaled_cot, contract_rows, preferred_element_type=jnp.float32
    ).astype(jnp.bfloat16)

    lead = weights[0] * weights[1] * (gate_sum[0] - gate_sum[1])
    logit_grad = (picked[0] - picked[1]) * lead[None, :]
    own_logit = lax.dynamic_slice_in_dim(logit_grad, ep_index * tok_rows, tok_rows, 1)
    gate_grad = lax.dynamic_slice_in_dim(gate_sum, ep_index * tok_rows, tok_rows, 1).T
    router_cols = lax.dynamic_slice_in_dim(router, tp_index * col_width, col_width, 0)
    token_grad = (
        routed_dx
        + lax.dot_general(
            own_logit,
            router_cols.astype(jnp.float32),
            (((0,), (1,)), ((), ())),
            precision=highest,
        )
    ).astype(jnp.bfloat16)
    seg = width // (ep_count * tp_count)
    own_cols = lax.dynamic_slice_in_dim(
        tok_all, (ep_index * tp_count + tp_index) * seg, seg, 1
    ).astype(jnp.float32)
    router_grad = lax.dot_general(
        logit_grad, own_cols, (((1,), (0,)), ((), ())), precision=highest
    ).T
    return (token_grad, gate_grad, grad_gate[None], grad_up[None], grad_down[None], router_grad)


def shards(tokens, cotangent, routes, router, w_gate, w_up, w_down):
    slots = 3 * routes.shape[1] * BLOCKS
    dense = slots >= lax.axis_size("ep") and lax.axis_size("tp") == 2 * CORES
    path = dense_shards if dense else routed_shards
    return path(tokens, cotangent, routes, router, w_gate, w_up, w_down)


def solution(mesh):
    placed = (
        P("ep", None),
        P("ep", None),
        P("ep", None),
        P(),
        P("ep", None, "tp"),
        P("ep", None, "tp"),
        P("ep", "tp", None),
    )
    return jax.shard_map(
        shards,
        mesh=mesh,
        in_specs=placed,
        out_specs=(
            P("ep", "tp"),
            P("ep", None),
            P("ep", None, "tp"),
            P("ep", None, "tp"),
            P("ep", "tp", None),
            P(("ep", "tp"), None),
        ),
        check_vma=False,
    )
```
